512 devices in a mesh: sp: 128 (over z, x, core), tp: 4 (over y).
Axes of the slice: x: 4, y: 4, z: 16, core: 2. Of those that a mesh axis runs over, the one named last changes fastest.
Arguments:
- hidden_in: bfloat16 [32768, 2048], P('sp'), may hold values from -8 to 8
- w_convb: bfloat16 [2048, 1024], P('sp', 'tp'), may hold values from -0.125 to 0.125
- w_convc: bfloat16 [2048, 1024], P('sp', 'tp'), may hold values from -0.125 to 0.125
- w_convx: bfloat16 [2048, 1024], P('sp', 'tp'), may hold values from -0.125 to 0.125
- w_query: bfloat16 [2048, 1024], P('sp', 'tp'), may hold values from -1 to 1
- w_key: bfloat16 [2048, 1024], P('sp', 'tp'), may hold values from -1 to 1
- w_value: bfloat16 [2048, 1024], P('sp', 'tp'), may hold values from -0.125 to 0.125
- conv_taps: float32 [3, 1024], P(None, 'tp'), may hold values from -3.5 to 3.5
- gate_cache: float32 [32768, 16], P(None, 'tp'), as said below
- w_out_conv: bfloat16 [1024, 2048], P('tp'), may hold values from -0.125 to 0.125
- w_out_attn: bfloat16 [1024, 2048], P('tp'), may hold values from -0.125 to 0.125
Outputs:
- mixed: bfloat16 [32768, 2048], P(('sp', 'tp'))
The draws below stay inside these ranges and needn't reach their ends.
Inputs may be any that keep to these rules, and one draw needn't show every extreme that they name: `gate_cache`: down each column, read from row 4096 to the last row and then from row 0 on, the values never rise.
All inputs are finite; a program needn't handle non-finite values.
Results may differ from the reference program's by a relative error of at most 0.018.
Values may be sent and summed in bfloat16 or wider, within the bound.
No kernel may reach another device: no remote copies, remote signals or barrier semaphores. Data moves between devices by JAX's collectives and lax.ppermute only.
A program may use at most 128 MiB of HBM per device.

```python
import math
import jax
import jax.numpy as jnp
from jax import lax

D = 2048
CONV = 1024
HEADS = 16
HD = 64
TOK_DEV = 256
STREAM_EXTENT = 8192
ROLL_ROWS = 4096
ATTW = 1024
ENTRIES_OVERALL = 32768
N_TP = 4


def weight_pairs(key):
    base = jnp.clip(jax.random.normal(jax.random.fold_in(key, 101), (D, HEADS * HD), jnp.float32), -8.0, 8.0)
    other = jnp.clip(jax.random.normal(jax.random.fold_in(key, 202), (D, HEADS * HD), jnp.float32), -8.0, 8.0)
    keyed = other
    factor = 1.7 * D ** (-0.5)
    return (base * factor, jnp.clip(keyed, -8.0, 8.0) * factor)


def draw_w_query(key, part):
    return weight_pairs(key)[0].astype(jnp.bfloat16)


def draw_w_key(key, part):
    return weight_pairs(key)[1].astype(jnp.bfloat16)


def draw_hidden_in(key, part):
    base = jax.random.normal(jax.random.fold_in(key, 1), (ENTRIES_OVERALL, D), jnp.float32)
    return jnp.clip(base, -8.0, 8.0).astype(jnp.bfloat16)


def draw_gate_cache(key, part):
    order = jax.random.permutation(jax.random.fold_in(key, 11), HEADS)
    slow_count = HEADS // 2
    slow = (order < slow_count).astype(jnp.float32)
    fast_rate = jnp.exp(jax.random.uniform(jax.random.fold_in(key, 12), (HEADS,), jnp.float32, math.log(1.0 / 100.0), math.log(1.0 / 30.0)))
    slow_rate = jax.random.uniform(jax.random.fold_in(key, 13), (HEADS,), jnp.float32, 0.3, 0.8) / STREAM_EXTENT
    rate = slow * slow_rate + (1.0 - slow) * fast_rate
    block_factor = jnp.exp(jax.random.uniform(jax.random.fold_in(key, 14), (ENTRIES_OVERALL // TOK_DEV, 1, HEADS), jnp.float32, math.log(0.5), math.log(2.0)))
    roughness = jax.random.uniform(jax.random.fold_in(key, 15), (ENTRIES_OVERALL // TOK_DEV, TOK_DEV, HEADS), jnp.float32, 0.3, 1.7)
    opening_scores = -(rate * block_factor * roughness).reshape(ENTRIES_OVERALL, HEADS)
    spike_clusters = jax.random.bernoulli(jax.random.fold_in(key, 16), 2.0 / STREAM_EXTENT, (ENTRIES_OVERALL, 1))
    objective_errors = jax.random.uniform(jax.random.fold_in(key, 17), (ENTRIES_OVERALL, HEADS), jnp.float32, math.log(0.5), math.log(0.8))
    opening_scores = opening_scores + jnp.where(spike_clusters, objective_errors, 0.0)
    return jnp.roll(jnp.cumsum(opening_scores, axis=0), ROLL_ROWS, axis=0)


def block_scale(own_key, dims, split, smallest, high):
    def one(axis_at, blocks):
        draws = jax.random.uniform(jax.random.fold_in(jax.random.fold_in(own_key, 6), axis_at), (blocks,), jnp.float32, smallest / len(split), high / len(split))
        return jnp.repeat(jnp.exp(draws), dims[axis_at] // blocks).reshape((-1,) + (1,) * (len(dims) - axis_at - 1))

    loudness = one(*split[0])
    for cut in split[1:]:
        loudness = loudness * one(*cut)
    return loudness


def scatter_about(stream_key, dims, spread, most, split=(), held_as=jnp.bfloat16):
    values = jax.random.normal(stream_key, dims, jnp.float32) * spread
    if len(split) > 0:
        values = block_scale(stream_key, dims, split, -0.22, 0.18) * values
    return jnp.clip(values, min=-most, max=most).astype(held_as)


def setup_inputs(seed: int = 0) -> dict:
    key_of = jax.random.split(jax.random.key(seed), 12)
    hidden_in = draw_hidden_in(jax.random.fold_in(key_of[11], 71), 0)
    w_convb = scatter_about(key_of[1], (D, CONV), D ** -0.5, 0.125, ((0, 128), (1, 4)))
    w_convc = scatter_about(key_of[2], (D, CONV), D ** -0.5, 0.125, ((0, 128), (1, 4)))
    w_convx = scatter_about(key_of[3], (D, CONV), D ** -0.5, 0.125, ((0, 128), (1, 4)))
    w_query = draw_w_query(jax.random.fold_in(key_of[11], 71), 0)
    w_key = draw_w_key(jax.random.fold_in(key_of[11], 71), 0)
    w_value = scatter_about(key_of[6], (D, ATTW), D ** -0.5, 0.125, ((0, 128), (1, 4)))
    conv_taps = scatter_about(key_of[7], (3, CONV), 3 ** -0.5, 3.5, ((1, 4),), jnp.float32)
    gate_cache = draw_gate_cache(jax.random.fold_in(key_of[11], 71), 0)
    w_out_conv = scatter_about(key_of[9], (CONV, D), (CONV + HEADS * HD) ** -0.5, 0.125, ((0, 4),))
    w_out_attn = scatter_about(key_of[10], (ATTW, D), (CONV + HEADS * HD) ** -0.5, 0.125, ((0, 4),))
    return {"hidden_in": hidden_in, "w_convb": w_convb, "w_convc": w_convc, "w_convx": w_convx, "w_query": w_query, "w_key": w_key, "w_value": w_value, "conv_taps": conv_taps, "gate_cache": gate_cache, "w_out_conv": w_out_conv, "w_out_attn": w_out_attn}


neg_large = -1e30


def project(hidden_in, weight):
    return jnp.dot(hidden_in, weight, preferred_element_type=jnp.float32).astype(jnp.bfloat16)


def short_conv(gate_b, gate_c, conv_values, conv_taps):
    conv_input = (gate_c.astype(jnp.float32) * conv_values.astype(jnp.float32)).astype(jnp.bfloat16)
    conv_input = lax.optimization_barrier(conv_input)
    framed = conv_input.reshape(-1, STREAM_EXTENT, CONV).astype(jnp.float32)
    padded = jnp.pad(framed, ((0, 0), (2, 0), (0, 0)))
    mixed_rows = conv_taps[0] * padded[:, :STREAM_EXTENT] + conv_taps[1] * padded[:, 1:STREAM_EXTENT + 1] + conv_taps[2] * padded[:, 2:]
    return (gate_b.astype(jnp.float32) * mixed_rows.reshape(-1, CONV)).astype(jnp.bfloat16)


def attention(query, keys, values, gate_cache):
    seq_count = query.shape[0] // STREAM_EXTENT

    def heads_first(array):
        return array.reshape(seq_count, STREAM_EXTENT, HEADS, HD).transpose(0, 2, 1, 3).reshape(seq_count * HEADS, STREAM_EXTENT, HD)

    query_heads = heads_first(query)
    key_heads = heads_first(keys)
    value_heads = heads_first(values)
    gate_heads = gate_cache.reshape(seq_count, STREAM_EXTENT, HEADS).transpose(0, 2, 1).reshape(seq_count * HEADS, STREAM_EXTENT)
    blocks = STREAM_EXTENT // TOK_DEV

    def one_block(flat):
        group = flat // blocks
        first_row = (flat % blocks) * TOK_DEV
        query_all = lax.dynamic_index_in_dim(query_heads, group, 0, False)
        key_all = lax.dynamic_index_in_dim(key_heads, group, 0, False)
        value_all = lax.dynamic_index_in_dim(value_heads, group, 0, False)
        gate_all = lax.dynamic_index_in_dim(gate_heads, group, 0, False)
        query_rows = lax.dynamic_slice_in_dim(query_all, first_row, TOK_DEV, 0)
        gate_rows = lax.dynamic_slice_in_dim(gate_all, first_row, TOK_DEV, 0)
        scores = jnp.dot(query_rows, key_all.T, preferred_element_type=jnp.float32) * (HD ** -0.5)
        scores = scores + gate_rows[:, None] - gate_all[None, :]
        row_pos = first_row + jnp.arange(TOK_DEV, dtype=jnp.int32)[:, None]
        col_pos = jnp.arange(STREAM_EXTENT, dtype=jnp.int32)[None, :]
        scores = jnp.where(col_pos <= row_pos, scores, neg_large)
        weights = jnp.exp(scores - jnp.max(scores, axis=1, keepdims=True))
        weights_low = weights.astype(jnp.bfloat16)
        summed = jnp.dot(weights_low, value_all, preferred_element_type=jnp.float32)
        return summed / jnp.sum(weights, axis=1, keepdims=True)

    outputs = lax.map(one_block, jnp.arange(seq_count * HEADS * blocks, dtype=jnp.int32))
    outputs = outputs.reshape(seq_count, HEADS, STREAM_EXTENT, HD).transpose(0, 2, 1, 3)
    return outputs.reshape(seq_count * STREAM_EXTENT, HEADS * HD).astype(jnp.bfloat16)


def reference(hidden_in, w_convb, w_convc, w_convx, w_query, w_key, w_value, conv_taps, gate_cache, w_out_conv, w_out_attn):
    hidden_in = jnp.roll(hidden_in, -ROLL_ROWS, axis=0)
    gate_cache = jnp.roll(gate_cache, -ROLL_ROWS, axis=0)
    gate_b = project(hidden_in, w_convb)
    gate_c = project(hidden_in, w_convc)
    conv_values = project(hidden_in, w_convx)
    query = project(hidden_in, w_query)
    keys = project(hidden_in, w_key)
    values = project(hidden_in, w_value)
    conv_out = short_conv(gate_b, gate_c, conv_values, conv_taps)
    attn_out = attention(query, keys, values, gate_cache)
    conv_group = CONV // N_TP
    attn_group = HEADS * HD // N_TP
    summed = jnp.zeros((hidden_in.shape[0], D), jnp.float32)
    for group in range(N_TP):
        value_partial = jnp.dot(conv_out[:, group * conv_group:(group + 1) * conv_group],
                          w_out_conv[group * conv_group:(group + 1) * conv_group],
                          preferred_element_type=jnp.float32)
        value_partial = value_partial + jnp.dot(attn_out[:, group * attn_group:(group + 1) * attn_group],
                                    w_out_attn[group * attn_group:(group + 1) * attn_group],
                                    preferred_element_type=jnp.float32)
        summed = summed + lax.optimization_barrier(value_partial.astype(jnp.bfloat16)).astype(jnp.float32)
    return jnp.roll(summed.astype(jnp.bfloat16), ROLL_ROWS, axis=0)
```

```python
import functools

import jax
import jax.numpy as jnp
from jax import lax
from jax.experimental import pallas as pl
from jax.experimental.pallas import tpu as pltpu
from jax.sharding import Mesh, PartitionSpec as P

LOG2E = 1.4426950408889634
NEG = -1e30
BLK = 256
bf16 = jnp.bfloat16
f32 = jnp.float32


def dot_t(a, b):
    return lax.dot_general(a, b, (((0,), (0,)), ((), ())), preferred_element_type=f32)


def attend_kernel(where, kv, q, gate, *refs, last):
    if last:
        acc_in, ml_in, out, kbuf, qbuf, acc, ml = refs
    else:
        acc, ml, kbuf, qbuf = refs
    core = where[0]
    xi = where[1]
    hd = kv.shape[3]
    aug = kbuf.shape[2]
    cb = 1 - core if last else core

    if last:
        acc[...] = acc_in[...]
        ml[...] = ml_in[...]
    else:
        acc[...] = jnp.zeros_like(acc)
        line = lax.broadcasted_iota(jnp.int32, ml.shape, 1)
        ml[...] = jnp.where(line == 0, NEG, 0.0)

    row = lax.broadcasted_iota(jnp.int32, (aug - hd, BLK), 0)
    ones = jnp.where(row < 3, 1.0, 0.0).astype(bf16)
    for j in range(4):
        qbuf[j, 0:hd, :] = q[j]
        qbuf[j, hd:aug, :] = ones
    first = gate[0:1, 0:1]
    for z in range(4):
        for x in range(4):
            b = (first - gate[pl.ds(z * 8 + x * 2 + cb, 1), :]) * LOG2E
            hi = b.astype(bf16).astype(f32)
            rest = b - hi
            mid = rest.astype(bf16).astype(f32)
            lo = rest - mid
            rows = jnp.where(row == 0, hi, jnp.where(row == 1, mid, jnp.where(row == 2, lo, 0.0)))
            kbuf[x, z, 0:hd, :] = kv[x, z, 0]
            kbuf[x, z, hd:aug, :] = rows.astype(bf16)

    def step(j, blocks, allowed=None):
        m = ml[j, 0:1, :]
        qj = qbuf[j]
        ss = [dot_t(kbuf[x, z], qj) for x, z in blocks]
        if allowed is not None:
            ss = [jnp.where(allowed, s, NEG) for s in ss]
        top = m
        for s in ss:
            top = jnp.maximum(top, jnp.max(s, axis=0, keepdims=True))
        factor = jnp.exp2(m - top)
        l = ml[j, 1:2, :] * factor
        total = acc[j] * factor
        for s, (x, z) in zip(ss, blocks):
            p = jnp.exp2(s - top)
            l = l + jnp.sum(p, axis=0, keepdims=True)
            total = total + lax.dot_general(
                kv[x, z, 1], p.astype(bf16), (((1,), (0,)), ((), ())), preferred_element_type=f32
            )
        ml[j, 0:1, :] = top
        ml[j, 1:2, :] = l
        acc[j] = total

    if not last:
        krow = lax.broadcasted_iota(jnp.int32, (BLK, BLK), 0)
        qcol = lax.broadcasted_iota(jnp.int32, (BLK, BLK), 1)
        for j in range(4):
            step(j, [(xi, j)], krow <= qcol)

    def chunk(t, _):
        second = (t >= 1).astype(jnp.int32)
        third = (t >= 3).astype(jnp.int32)
        z = t - second - 2 * third
        step(1 + second + third, [(x, z) for x in range(4)])
        return 0

    lax.fori_loop(0, 6, chunk, 0)

    def pair(x, _):
        for j in range(4):
            step(j, [(x, j)])
        return 0

    lax.fori_loop(0, xi + core if last else xi, pair, 0)
    if last:
        for j in range(4):
            out[j] = (acc[j] / ml[j, 1:2, :]).astype(bf16)


def attend(where, kv, q, gate, state=None):
    hd = kv.shape[3]
    aug = hd + 16
    last = state is not None
    vmem = pl.BlockSpec(memory_space=pltpu.VMEM)
    smem = pl.BlockSpec(memory_space=pltpu.SMEM)
    held = [pltpu.VMEM((4, hd, BLK), f32), pltpu.VMEM((4, 8, BLK), f32)]
    carried = (jax.ShapeDtypeStruct((4, hd, BLK), f32), jax.ShapeDtypeStruct((4, 8, BLK), f32))
    return pl.pallas_call(
        functools.partial(attend_kernel, last=last),
        out_shape=jax.ShapeDtypeStruct((4, hd, BLK), bf16) if last else carried,
        in_specs=[smem, vmem, vmem, vmem] + ([vmem, vmem] if last else []),
        out_specs=vmem if last else (vmem, vmem),
        scratch_shapes=[pltpu.VMEM((4, 4, aug, BLK), bf16), pltpu.VMEM((4, aug, BLK), bf16)] + (held if last else []),
        cost_estimate=pl.CostEstimate(flops=2 * 10**9, bytes_accessed=2 * 10**6, transcendentals=10**6),
        name="attend_last" if last else "attend_first",
    )(where, kv, q, gate, *(state or ()))


def shards(
    hidden_in, w_convb, w_convc, w_convx, w_query, w_key, w_value, conv_taps, gate_cache, w_out_conv, w_out_attn
):
    zi = lax.axis_index("z")
    xi = lax.axis_index("x")
    ci = lax.axis_index("c")
    z_len = lax.axis_size("z")
    tok, width = hidden_in.shape
    rows, ch = w_convb.shape
    hd = w_query.shape[1] // 4
    per = hd + hd // 2
    half = ch // 2
    north = ci == 0
    place = (zi - 2) % 4
    cubes = [[(2 + 4 * g + i) % z_len for i in range(4)] for g in range(z_len // 4)]
    cubes_c = [[2 * z + c for z in cube for c in range(2)] for cube in cubes]
    swap = [(0, 1), (1, 0)]

    wq = w_query.reshape(rows, 4, hd)
    wk = w_key.reshape(rows, 4, hd)
    wv = w_value.reshape(rows, 4, hd)
    halves = []
    for c, w in enumerate((wk, wv)):
        heads = jnp.concatenate([w, wq[:, :, c * hd // 2 : (c + 1) * hd // 2]], axis=2).reshape(rows, 4 * per)
        convs = [w[:, c * half : (c + 1) * half] for w in (w_convb, w_convc, w_convx)]
        halves.append(jnp.concatenate([heads] + convs, axis=1))
    mine = jnp.where(north, halves[0], halves[1])
    theirs = lax.ppermute(jnp.where(north, halves[1], halves[0]), "c", swap)
    other = lax.ppermute(hidden_in, "c", swap)
    total = z_len * 8
    before = lax.ppermute(
        hidden_in[tok - 16 :], ("z", "x", "c"), [(i, (i + 1) % total) for i in range(total)]
    )
    w_rows = jnp.where(
        north, jnp.concatenate([mine, theirs], axis=0), jnp.concatenate([theirs, mine], axis=0)
    )
    w_all = lax.all_gather(w_rows, "z", axis=0, tiled=True)

    def over_x(w):
        w = lax.all_to_all(jnp.broadcast_to(w[None], (4,) + w.shape), "x", 0, 0, tiled=True)
        w = w.reshape(4, z_len, 2 * rows, w.shape[2]).transpose(1, 0, 2, 3)
        return w.reshape(width, w.shape[3])

    w_attn = over_x(w_all[:, : 4 * per])
    w_late, w_attn = lax.optimization_barrier((w_all[:, 4 * per :], w_attn))
    conv_mine = over_x(w_late)
    conv_theirs = lax.ppermute(conv_mine, "c", swap)

    tokens = jnp.concatenate([hidden_in, other], axis=0)
    proj = lax.dot_general(w_attn, tokens, (((0,), (1,)), ((), ())), preferred_element_type=f32)
    proj = proj.reshape(4, per, 2, tok)
    scale = jnp.where(jnp.arange(per) < hd, 1.0, LOG2E * hd**-0.5).astype(f32)
    proj = (proj * scale[None, :, None, None]).astype(bf16).transpose(0, 2, 1, 3)
    proj = jnp.where(north, proj, proj[:, ::-1]).reshape(8, per, tok)
    proj = lax.all_to_all(proj, ("z", "c"), 0, 0, tiled=True, axis_index_groups=cubes_c)
    proj = proj.reshape(4, 2, per, tok)
    q = proj[:, :, hd:].reshape(4, hd, tok)
    kv = proj[:, :, :hd]
    kv_own = lax.all_to_all(jnp.broadcast_to(kv[None], (4,) + kv.shape), "x", 0, 0, tiled=True)
    kv_own = kv_own.reshape(4, 4, 2, hd, tok)
    kv_oth = lax.ppermute(kv_own, "c", swap)

    gates = gate_cache.T
    stream = 32 * tok
    first = ((zi - place) % z_len) * 8 * tok
    low = lax.dynamic_slice(gates, (place, first), (1, stream // 2))
    high = lax.dynamic_slice(gates, (place, (first + stream // 2) % gates.shape[1]), (1, stream // 2))
    gate = jnp.concatenate([low, high], axis=1).reshape(32, tok)
    where = jnp.stack([ci, xi]).astype(jnp.int32)
    state = attend(where, kv_own, q, gate)
    heads = attend(where, kv_oth, q, gate, state)
    heads = lax.all_to_all(heads, "z", 0, 0, tiled=True, axis_index_groups=cubes)
    attn_out = heads.reshape(4 * hd, tok)

    longer = jnp.concatenate([before, hidden_in], axis=0)
    opening = (place == 0) & (xi == 0) & north
    keep = (jnp.arange(16 + tok)[:, None] >= 16) | jnp.logical_not(opening)

    def convolved(w, taps):
        trio = jnp.dot(longer, w, preferred_element_type=f32).astype(bf16).astype(f32)
        conv_input = (trio[:, half : 2 * half] * trio[:, 2 * half :]).astype(bf16).astype(f32)
        conv_input = jnp.where(keep, conv_input, 0.0)
        mixed_conv = (
            taps[0] * conv_input[14 : 14 + tok] + taps[1] * conv_input[15 : 15 + tok] + taps[2] * conv_input[16:]
        )
        return (trio[16:, :half] * mixed_conv).astype(bf16)

    taps0, taps1 = (conv_taps[:, :half], conv_taps[:, half:])
    conv_a = convolved(conv_mine, jnp.where(north, taps0, taps1))
    conv_b = convolved(conv_theirs, jnp.where(north, taps1, taps0))
    conv_out = jnp.where(
        north, jnp.concatenate([conv_a, conv_b], axis=1), jnp.concatenate([conv_b, conv_a], axis=1)
    )

    partial = jnp.dot(conv_out, w_out_conv, preferred_element_type=f32) + dot_t(attn_out, w_out_attn)
    partial = partial.astype(bf16).reshape(4, tok // 4, width)
    blocks = lax.all_to_all(partial, "y", 0, 0, tiled=True)
    return jnp.sum(blocks.astype(f32), axis=0).astype(bf16)


def solution(mesh):
    shape = mesh.devices.shape
    fine = Mesh(mesh.devices.reshape(shape[0] // 8, 4, 2, shape[1]), ("z", "x", "c", "y"))
    sp = ("z", "x", "c")
    return jax.shard_map(
        shards,
        mesh=fine,
        in_specs=(
            P(sp, None),
            P(sp, "y"),
            P(sp, "y"),
            P(sp, "y"),
            P(sp, "y"),
            P(sp, "y"),
            P(sp, "y"),
            P(None, "y"),
            P(None, "y"),
            P("y", None),
            P("y", None),
        ),
        out_specs=P(sp + ("y",), None),
        check_vma=False,
    )
```

```python
import functools

import jax
import jax.numpy as jnp
from jax import lax
from jax.experimental import pallas as pl
from jax.experimental.pallas import tpu as pltpu
from jax.sharding import Mesh, PartitionSpec as P

LOG2E = 1.4426950408889634
NEG = -1e30
BLK = 256
bf16 = jnp.bfloat16
f32 = jnp.float32


def dot_t(a, b):
    return lax.dot_general(a, b, (((0,), (0,)), ((), ())), preferred_element_type=f32)


def dot(a, b):
    return lax.dot_general(a, b, (((1,), (0,)), ((), ())), preferred_element_type=f32)


def prepare_kernel(where, b, c, x, q, k, v, mine, theirs):
    core = where[0]
    heads = k.shape[1]
    half = heads // 2
    lane = lax.broadcasted_iota(jnp.int32, (heads, half), 0)
    col = lax.broadcasted_iota(jnp.int32, (heads, half), 1)

    def fill(out, side):
        pick = jnp.where(lane == (col // 32) * 64 + col % 32 + side * 32, 1.0, 0.0).astype(bf16)
        keep = jnp.broadcast_to(side, (k.shape[0], heads)) == 0
        out[:, 0:heads] = jnp.where(keep, k[...].astype(f32), v[...].astype(f32)).astype(bf16)
        out[:, heads : heads + half] = dot(q[...], pick).astype(bf16)
        at = heads + half
        for w in (b, c, x):
            both = jnp.where(keep[:, :half], w[:, :half].astype(f32), w[:, half:].astype(f32))
            out[:, at : at + half] = both.astype(bf16)
            at += half

    fill(mine, core)
    fill(theirs, 1 - core)


def prepare(where, *ws):
    rows, heads = ws[0].shape
    vmem = pl.BlockSpec(memory_space=pltpu.VMEM)
    shape = jax.ShapeDtypeStruct((rows, 3 * heads), bf16)
    return pl.pallas_call(
        prepare_kernel,
        out_shape=(shape, shape),
        in_specs=[pl.BlockSpec(memory_space=pltpu.SMEM)] + [vmem] * 6,
        out_specs=(vmem, vmem),
        name="prepare",
    )(where, *ws)


def ordered(w, wbuf):
    piece = w.shape[1] // 16
    for x in range(4):
        for z in range(16):
            at = (z * 4 + x) * piece
            wbuf[at : at + piece, :] = w[x, z * piece : (z + 1) * piece, :]


def project_kernel(where, w, own, oth, out, wbuf):
    core = where[0]
    hd = 64
    ordered(w, wbuf)
    for hidden, slot in ((own, core), (oth, 1 - core)):
        cols = dot(hidden[...], wbuf[...]).T
        for i in range(4):
            at = 4 * hd + i * hd // 2
            out[2 * i + slot, 0:hd, :] = cols[i * hd : (i + 1) * hd].astype(bf16)
            scaled = cols[at : at + hd // 2] * (LOG2E * hd**-0.5)
            out[2 * i + slot, hd : hd + hd // 2, :] = scaled.astype(bf16)


def project(where, w, own, oth):
    vmem = pl.BlockSpec(memory_space=pltpu.VMEM)
    return pl.pallas_call(
        project_kernel,
        out_shape=jax.ShapeDtypeStruct((8, 96, own.shape[0]), bf16),
        in_specs=[pl.BlockSpec(memory_space=pltpu.SMEM)] + [vmem] * 3,
        out_specs=vmem,
        scratch_shapes=[pltpu.VMEM((own.shape[1], w.shape[2]), bf16)],
        cost_estimate=pl.CostEstimate(flops=8 * 10**8, bytes_accessed=4 * 10**6, transcendentals=0),
        name="project",
    )(where, w, own, oth)


def convolve_kernel(where, w, hidden, before, taps, out, wbuf, line, *, swapped):
    tok = hidden.shape[0]
    lead = before.shape[0]
    half = out.shape[1]
    side = 1 - where[0] if swapped else where[0]
    ordered(w, wbuf)
    opening = where[2] == 1
    trio = dot(hidden[...], wbuf[...]).astype(bf16).astype(f32)
    edge = dot(before[...], wbuf[:, half:]).astype(bf16).astype(f32)
    first = (edge[:, :half] * edge[:, half:]).astype(bf16).astype(f32)
    line[0:lead, :] = jnp.where(jnp.broadcast_to(opening, first.shape), 0.0, first)
    line[lead : lead + tok, :] = (trio[:, half : 2 * half] * trio[:, 2 * half :]).astype(bf16).astype(f32)
    keep = jnp.broadcast_to(side, (3, half)) == 0
    tap = jnp.where(keep, taps[:, :half], taps[:, half:])
    mixed = (
        tap[0:1] * line[lead - 2 : lead - 2 + tok, :]
        + tap[1:2] * line[lead - 1 : lead - 1 + tok, :]
        + tap[2:3] * line[lead : lead + tok, :]
    )
    out[...] = (trio[:, :half] * mixed).astype(bf16)


def convolve(where, w, hidden, before, taps, swapped):
    vmem = pl.BlockSpec(memory_space=pltpu.VMEM)
    tok, width = hidden.shape
    half = taps.shape[1] // 2
    return pl.pallas_call(
        functools.partial(convolve_kernel, swapped=swapped),
        out_shape=jax.ShapeDtypeStruct((tok, half), bf16),
        in_specs=[pl.BlockSpec(memory_space=pltpu.SMEM)] + [vmem] * 4,
        out_specs=vmem,
        scratch_shapes=[
            pltpu.VMEM((width, w.shape[2]), bf16),
            pltpu.VMEM((tok + before.shape[0], half), f32),
        ],
        cost_estimate=pl.CostEstimate(flops=4 * 10**8, bytes_accessed=3 * 10**6, transcendentals=0),
        name="convolve_oth" if swapped else "convolve_own",
    )(where, w, hidden, before, taps)


def attend_kernel(where, kv, q, gate, *refs, last):
    if last:
        acc_in, ml_in, out, kbuf, qbuf, acc, ml = refs
    else:
        acc, ml, kbuf, qbuf = refs
    core = where[0]
    xi = where[1]
    hd = kv.shape[3]
    aug = qbuf.shape[1]
    cb = 1 - core if last else core

    if last:
        acc[...] = acc_in[...]
        ml[...] = ml_in[...]
    else:
        acc[...] = jnp.zeros_like(acc)
        line = lax.broadcasted_iota(jnp.int32, ml.shape, 1)
        ml[...] = jnp.where(line == 0, NEG, 0.0)

    row = lax.broadcasted_iota(jnp.int32, (aug - hd, BLK), 0)
    ones = jnp.where(row < 3, 1.0, 0.0).astype(bf16)
    for j in range(4):
        qbuf[j, 0:hd, :] = q[j]
        qbuf[j, hd:aug, :] = ones
    first = gate[0:1, 0:1]
    for z in range(4):
        for x in range(4):
            b = (first - gate[pl.ds(z * 8 + x * 2 + cb, 1), :]) * LOG2E
            hi = b.astype(bf16).astype(f32)
            rest = b - hi
            mid = rest.astype(bf16).astype(f32)
            lo = rest - mid
            rows = jnp.where(row == 0, hi, jnp.where(row == 1, mid, jnp.where(row == 2, lo, 0.0)))
            cols = jnp.concatenate([kv[x, z, 0].astype(f32), rows], axis=0)
            kbuf[x, z] = cols.T.astype(bf16)

    def steps(work, allowed=None):
        old = [(ml[j, 0:1, :], ml[j, 1:2, :], acc[j]) for j, _ in work]
        scores = []
        for j, blocks in work:
            qj = qbuf[j]
            ss = [dot(kbuf[x, z], qj) for x, z in blocks]
            scores.append(ss if allowed is None else [jnp.where(allowed, s, NEG) for s in ss])
        new = []
        for (j, blocks), ss, (m, l, total) in zip(work, scores, old):
            top = m
            for s in ss:
                top = jnp.maximum(top, jnp.max(s, axis=0, keepdims=True))
            factor = jnp.exp2(m - top)
            l = l * factor
            total = total * factor
            for s, (x, z) in zip(ss, blocks):
                p = jnp.exp2(s - top)
                l = l + jnp.sum(p, axis=0, keepdims=True)
                total = total + dot(kv[x, z, 1], p.astype(bf16))
            new.append((top, l, total))
        for (j, _), (top, l, total) in zip(work, new):
            ml[j, 0:1, :] = top
            ml[j, 1:2, :] = l
            acc[j] = total

    if not last:
        krow = lax.broadcasted_iota(jnp.int32, (BLK, BLK), 0)
        qcol = lax.broadcasted_iota(jnp.int32, (BLK, BLK), 1)
        steps([(j, [(xi, j)]) for j in range(4)], krow <= qcol)

    def chunk(t, _):
        second = (t >= 1).astype(jnp.int32)
        third = (t >= 3).astype(jnp.int32)
        z = t - second - 2 * third
        steps([(1 + second + third, [(x, z) for x in range(4)])])
        return 0

    lax.fori_loop(0, 6, chunk, 0)

    def pair(x, _):
        steps([(j, [(x, j)]) for j in range(4)])
        return 0

    lax.fori_loop(0, xi + core if last else xi, pair, 0)
    if last:
        for j in range(4):
            out[j] = (acc[j] / ml[j, 1:2, :]).astype(bf16)


def attend(where, kv, q, gate, state=None):
    hd = kv.shape[3]
    aug = 2 * hd
    last = state is not None
    vmem = pl.BlockSpec(memory_space=pltpu.VMEM)
    smem = pl.BlockSpec(memory_space=pltpu.SMEM)
    held = [pltpu.VMEM((4, hd, BLK), f32), pltpu.VMEM((4, 8, BLK), f32)]
    carried = (jax.ShapeDtypeStruct((4, hd, BLK), f32), jax.ShapeDtypeStruct((4, 8, BLK), f32))
    return pl.pallas_call(
        functools.partial(attend_kernel, last=last),
        out_shape=jax.ShapeDtypeStruct((4, hd, BLK), bf16) if last else carried,
        in_specs=[smem, vmem, vmem, vmem] + ([vmem, vmem] if last else []),
        out_specs=vmem if last else (vmem, vmem),
        scratch_shapes=[pltpu.VMEM((4, 4, BLK, aug), bf16), pltpu.VMEM((4, aug, BLK), bf16)] + (held if last else []),
        cost_estimate=pl.CostEstimate(flops=2 * 10**9, bytes_accessed=2 * 10**6, transcendentals=10**6),
        name="attend_last" if last else "attend_first",
    )(where, kv, q, gate, *(state or ()))


def shards(
    hidden_in, w_convb, w_convc, w_convx, w_query, w_key, w_value, conv_taps, gate_cache, w_out_conv, w_out_attn
):
    zi = lax.axis_index("z")
    xi = lax.axis_index("x")
    ci = lax.axis_index("c")
    z_len = lax.axis_size("z")
    tok, width = hidden_in.shape
    rows, ch = w_convb.shape
    hd = w_query.shape[1] // 4
    half = ch // 2
    north = ci == 0
    place = (zi - 2) % 4
    cubes = [[(2 + 4 * g + i) % z_len for i in range(4)] for g in range(z_len // 4)]
    cubes_c = [[2 * z + c for z in cube for c in range(2)] for cube in cubes]
    swap = [(0, 1), (1, 0)]
    opening = (place == 0) & (xi == 0) & north
    where = jnp.stack([ci, xi, opening.astype(jnp.int32)]).astype(jnp.int32)

    mine, theirs = prepare(where, w_convb, w_convc, w_convx, w_query, w_key, w_value)
    theirs = lax.ppermute(theirs, "c", swap)
    other = lax.ppermute(hidden_in, "c", swap)
    total = z_len * 8
    before = lax.ppermute(
        hidden_in[tok - 16 :], ("z", "x", "c"), [(i, (i + 1) % total) for i in range(total)]
    )
    w_rows = jnp.where(
        north, jnp.concatenate([mine, theirs], axis=0), jnp.concatenate([theirs, mine], axis=0)
    )
    w_all = lax.all_gather(w_rows, "z", axis=0, tiled=True)

    def over_x(w):
        return lax.all_to_all(jnp.broadcast_to(w[None], (4,) + w.shape), "x", 0, 0, tiled=True)

    w_attn = over_x(w_all[:, : ch + half])
    proj = project(where, w_attn, hidden_in, other)
    proj = lax.all_to_all(proj, ("z", "c"), 0, 0, tiled=True, axis_index_groups=cubes_c)
    proj = proj.reshape(4, 2, hd + hd // 2, tok)
    q = proj[:, :, hd:].reshape(4, hd, tok)
    kv = proj[:, :, :hd]
    kv_own = over_x(kv).reshape(4, 4, 2, hd, tok)
    w_late, kv_own = lax.optimization_barrier((w_all[:, ch + half :], kv_own))
    conv_mine = over_x(w_late)
    kv_oth = lax.ppermute(kv_own, "c", swap)

    gates = gate_cache.T
    stream = 32 * tok
    first = ((zi - place) % z_len) * 8 * tok
    low = lax.dynamic_slice(gates, (place, first), (1, stream // 2))
    high = lax.dynamic_slice(gates, (place, (first + stream // 2) % gates.shape[1]), (1, stream // 2))
    gate = jnp.concatenate([low, high], axis=1).reshape(32, tok)
    state = attend(where, kv_own, q, gate)
    heads = attend(where, kv_oth, q, gate, state)
    conv_mine, heads = lax.optimization_barrier((conv_mine, heads))
    heads = lax.all_to_all(heads, "z", 0, 0, tiled=True, axis_index_groups=cubes)
    attn_out = heads.reshape(4 * hd, tok)

    conv_theirs = lax.ppermute(conv_mine, "c", swap)
    conv_a = convolve(where, conv_mine, hidden_in, before, conv_taps, False)
    conv_b = convolve(where, conv_theirs, hidden_in, before, conv_taps, True)
    conv_out = jnp.where(
        north, jnp.concatenate([conv_a, conv_b], axis=1), jnp.concatenate([conv_b, conv_a], axis=1)
    )

    partial = jnp.dot(conv_out, w_out_conv, preferred_element_type=f32) + dot_t(attn_out, w_out_attn)
    partial = partial.astype(bf16).reshape(4, tok // 4, width)
    blocks = lax.all_to_all(partial, "y", 0, 0, tiled=True)
    return jnp.sum(blocks.astype(f32), axis=0).astype(bf16)


def solution(mesh):
    shape = mesh.devices.shape
    fine = Mesh(mesh.devices.reshape(shape[0] // 8, 4, 2, shape[1]), ("z", "x", "c", "y"))
    sp = ("z", "x", "c")
    return jax.shard_map(
        shards,
        mesh=fine,
        in_specs=(
            P(sp, None),
            P(sp, "y"),
            P(sp, "y"),
            P(sp, "y"),
            P(sp, "y"),
            P(sp, "y"),
            P(sp, "y"),
            P(None, "y"),
            P(None, "y"),
            P("y", None),
            P("y", None),
        ),
        out_specs=P(sp + ("y",), None),
        check_vma=False,
    )
```
